128 devices in a mesh: ep: 16 (over z, x), tp: 8 (over y, core).
Axes of the slice: x: 4, y: 4, z: 4, core: 2. Of those that a mesh axis runs over, the one named last changes fastest.
Arguments:
- mix_tokens: bfloat16 [16384, 2048], P('ep'), may hold values from -6 to 6
- mix_gain: float32 [2048], replicated, may hold values from 0.1 to 1.9
- w_query: bfloat16 [2048, 2048], P(None, 'tp'), may hold values from -0.125 to 0.125
- w_forget_fwd: bfloat16 [2048, 2048], P(None, 'tp'), may hold values from -0.125 to 0.125
- w_forget_bwd: bfloat16 [2048, 2048], P(None, 'tp'), may hold values from -0.125 to 0.125
- w_value: bfloat16 [2048, 2048], P(None, 'tp'), may hold values from -0.125 to 0.125
- decay_floor: float32 [2048], P('tp'), may hold values from 0.975 to 1
- decay_shift: float32 [16384, 16], P('ep', 'tp'), may hold values from -1.3 to 0
- head_gain: float32 [128], replicated, may hold values from 0.1 to 1.9
- w_out: bfloat16 [2048, 2048], replicated, may hold values from -0.125 to 0.125
- moe_tokens: bfloat16 [6144, 2048], P('ep'), may hold values from -6 to 6
- moe_gain: float32 [2048], replicated, may hold values from 0.1 to 1.9
- routes: int32 [6144, 2], P('ep'), may hold values from 0 to 15, all different within a row; in each aligned block of 384 rows (0 to 383, 384 to 767, ...) at most 72 rows name the same one
- route_logits: float32 [6144, 2], P('ep'), may hold values from -6 to 6
- w_expert_gate: bfloat16 [16, 2048, 5120], P('ep', None, 'tp'), may hold values from -0.125 to 0.125
- w_expert_up: bfloat16 [16, 2048, 5120], P('ep', None, 'tp'), may hold values from -0.125 to 0.125
- w_expert_down: bfloat16 [16, 5120, 2048], P('ep', 'tp'), may hold values from -0.078125 to 0.078125
Outputs:
- mixed_out: bfloat16 [16384, 2048], P(('ep', 'tp'))
- moe_out: bfloat16 [6144, 2048], P('ep', 'tp')
The draws below stay inside these ranges and needn't reach their ends.
Inputs may be any that keep to these rules, and one draw needn't show every extreme that they name: `routes`: in each aligned block of 384 rows (the rows of one index of ep) no expert is named by more than 72 rows, and in some block an expert is named by exactly 72; the two entries of a row differ.
All inputs are finite; a program needn't handle non-finite values.
Results may differ from the reference program's by a relative error of at most 0.014.
Values may be sent and summed in bfloat16 or wider, within the bound.
A program may use at most 128 MiB of HBM per device.

```python
import functools
import math
import jax
import jax.numpy as jnp
import numpy as np
from jax import lax

D = 2048
HEADS = 16
DK = 128
DV = 128
FF = 5120
TOPK = 2
M_EP = 384
SEG = 1024
ROWS = 16384
MROWS = 6144
EXPERTS = 16
CAP = 72
N_EP = 16
N_TP = 8


def decay_table(key):
    head_key = jax.random.fold_in(key, 11)
    scores = jax.random.randint(jax.random.fold_in(head_key, 1), (HEADS,), 0, 1000)
    forced = jax.random.randint(jax.random.fold_in(head_key, 2), (), 0, HEADS)
    limit = 500
    return (scores < limit) | (jnp.arange(HEADS) == forced)


def draw_decay_floor(key, part):
    fast = decay_table(key)
    rate = jnp.where(fast, 1.0 / 40.0, 0.2 / ROWS).astype(jnp.float32)
    spread = jax.random.uniform(jax.random.fold_in(key, 21), (HEADS, DK), jnp.float32, 0.5, 1.0)
    return (1.0 - rate[:, None] * spread).reshape(HEADS * DK)


def draw_decay_shift(key, part):
    fast = decay_table(key)
    start_offset = jnp.where(fast, 1.0 / 40.0, 0.25 / ROWS).astype(jnp.float32)
    block_total = ROWS // SEG
    factor = jnp.exp(jax.random.uniform(jax.random.fold_in(key, 31), (block_total, HEADS), jnp.float32, math.log(0.5), math.log(2.0)))
    row_amounts = jnp.repeat(factor, SEG, axis=0)
    slot_locations = jax.random.randint(jax.random.fold_in(key, 32), (2, HEADS), 0, ROWS)
    loss_values = jax.random.uniform(jax.random.fold_in(key, 33), (2, HEADS), jnp.float32, 0.2, 0.45)
    row_identifiers = jnp.arange(ROWS)[:, None]
    token_groups = jnp.where(row_identifiers == slot_locations[0][None, :], jnp.log1p(-loss_values[0])[None, :], 0.0) + jnp.where(row_identifiers == slot_locations[1][None, :], jnp.log1p(-loss_values[1])[None, :], 0.0)
    return (-start_offset[None, :] * row_amounts + token_groups).astype(jnp.float32)


def block_levels(rng, shape, shards, low, top_value):
    def one(dim, blocks):
        heights = jax.random.uniform(jax.random.fold_in(jax.random.fold_in(rng, 6), dim), (blocks,), jnp.float32, low / len(shards), top_value / len(shards))
        return jnp.repeat(jnp.exp(heights), shape[dim] // blocks).reshape((-1,) + (1,) * (len(shape) - dim - 1))

    loudness = one(*shards[0])
    for cut in shards[1:]:
        loudness = loudness * one(*cut)
    return loudness


def shared_out(own_key, own, number, rows, number_of, top, bound, skew):
    ranking = jax.random.permutation(own_key, number_of)
    packed, common = load_shares(number_of, rows * top, bound, skew, True), load_shares(number_of, rows * top, bound, skew, False)
    places = jnp.arange(number_of)

    def named(lengths, offset_by):
        used = int((lengths > 0).sum())
        fixed = max(1, used // 4)
        passed = fixed + (places - fixed + offset_by * (used - fixed)) % max(1, number_of - fixed)
        return jnp.zeros((number_of,), jnp.int32).at[ranking[jnp.where(places < fixed, places, passed)]].set(jnp.asarray(lengths, jnp.int32))

    lengths = jnp.where(number % 4 == 0, named(packed, number // 4), named(common, number - number // 4 - 1))
    mixed = jax.random.permutation(jax.random.fold_in(own, 3), number_of)
    donor, sink = mixed[0:number_of // 2 * 2:2], mixed[1:number_of // 2 * 2:2]
    slack = jnp.minimum(lengths[donor] - 1, bound - lengths[sink]) // 2
    slack = jnp.where((donor == ranking[0]) | (sink == ranking[0]) | (lengths[sink] == 0), 0, jnp.maximum(slack, 0))
    passed = jax.random.randint(jax.random.fold_in(own, 4), (number_of // 2,), 0, 1 << 20) % (slack + 1)
    lengths = lengths.at[donor].add(-passed).at[sink].add(passed)
    labels = jnp.searchsorted(jnp.cumsum(lengths), jnp.arange(rows * top), side="right").astype(jnp.int32)
    listing = labels.reshape(top, rows).T
    listing = listing[jax.random.permutation(jax.random.fold_in(own, 1), rows)]
    offset_by = jax.random.randint(jax.random.fold_in(own, 2), (rows, 1), 0, top)
    return jnp.take_along_axis(listing, (jnp.arange(top)[None, :] + offset_by) % top, axis=1)


def load_shares(count, total, reach, lean, full):
    portions = [(1 << 20) // math.isqrt(rank ** lean) + 1 for rank in range(1, count + 1)]
    largest = reach if full else min(reach, max(-(-total // count), total * portions[0] // sum(portions)))
    least = 1 if total - largest >= count - 1 else 0
    holding, surplus = [largest] + [least] * (count - 1), total - largest - least * (count - 1)
    while surplus > 0:
        free = [i for i in range(1, count) if holding[i] < largest] or [i for i in range(1, count) if holding[i] < reach]
        whole, remaining = sum([portions[i] for i in free]), surplus
        for i in free:
            more = min(reach - holding[i], max(1, remaining * portions[i] // whole), surplus)
            holding[i] = holding[i] + more
            surplus = surplus - more
    return np.array(holding)


def gaussian(key, shape, scale, most, cuts=(), held_as=jnp.bfloat16):
    values = scale * jax.random.normal(key, shape, jnp.float32)
    if cuts:
        values = values * block_levels(key, shape, cuts, -0.22, 0.18)
    return jnp.clip(values, -most, most).astype(held_as)


def setup_inputs(seed: int = 0) -> dict:
    splits = jax.random.split(jax.random.key(seed), 18)
    mix_tokens = gaussian(splits[0], (ROWS, D), 1.0, 6.0, ((0, 16),))
    mix_gain = jnp.clip(1.0 + 0.18 * jax.random.normal(splits[1], (D,), jnp.float32), 0.1, 1.9)
    w_query = gaussian(splits[2], (D, HEADS * DK), D ** -0.5, 0.125, ((1, 8),))
    w_forget_fwd = gaussian(splits[3], (D, HEADS * DK), D ** -0.5, 0.125, ((1, 8),))
    w_forget_bwd = gaussian(splits[4], (D, HEADS * DK), D ** -0.5, 0.125, ((1, 8),))
    w_value = gaussian(splits[5], (D, HEADS * DV), D ** -0.5, 0.125, ((1, 8),))
    decay_floor = draw_decay_floor(jax.random.fold_in(splits[17], 71), 0)
    decay_shift = draw_decay_shift(jax.random.fold_in(splits[17], 71), 0)
    head_gain = jnp.clip(1.0 + 0.18 * jax.random.normal(splits[8], (DV,), jnp.float32), 0.1, 1.9)
    w_out = gaussian(splits[9], (HEADS * DV, D), D ** -0.5, 0.125)
    moe_tokens = gaussian(splits[10], (MROWS, D), 1.0, 6.0, ((0, 16),))
    moe_gain = jnp.clip(1.0 + 0.18 * jax.random.normal(splits[11], (D,), jnp.float32), 0.1, 1.9)
    routes_keys = jax.random.split(jax.random.fold_in(splits[12], 1), MROWS // M_EP)
    routes_turns = jax.random.permutation(jax.random.fold_in(splits[12], 3), MROWS // M_EP)
    routes = jax.vmap(lambda own, number: shared_out(jax.random.fold_in(splits[12], 2), own, number, M_EP, EXPERTS, 2, CAP, 1))(routes_keys, routes_turns).reshape((MROWS, TOPK))
    route_logits = gaussian(splits[13], (MROWS, TOPK), 1.5, 6.0, ((0, 16),), jnp.float32)
    w_expert_gate = gaussian(splits[14], (EXPERTS, D, FF), D ** -0.5, 0.125, ((0, 16), (2, 8)))
    w_expert_up = gaussian(splits[15], (EXPERTS, D, FF), D ** -0.5, 0.125, ((0, 16), (2, 8)))
    w_expert_down = gaussian(splits[16], (EXPERTS, FF, D), FF ** -0.5, 0.078125, ((0, 16), (1, 8)))
    return {"mix_tokens": mix_tokens, "mix_gain": mix_gain, "w_query": w_query, "w_forget_fwd": w_forget_fwd, "w_forget_bwd": w_forget_bwd, "w_value": w_value, "decay_floor": decay_floor, "decay_shift": decay_shift, "head_gain": head_gain, "w_out": w_out, "moe_tokens": moe_tokens, "moe_gain": moe_gain, "routes": routes, "route_logits": route_logits, "w_expert_gate": w_expert_gate, "w_expert_up": w_expert_up, "w_expert_down": w_expert_down}


EPSILON = 1e-06
PRECISE = lax.Precision.HIGHEST

def rms_rows(array, norm_gain):
    floats = array.astype(jnp.float32)
    factor = lax.rsqrt(lax.optimization_barrier(jnp.mean(floats * floats, axis=-1, keepdims=True)) + EPSILON)
    return floats * factor * norm_gain

def decay_terms(pre_act, lower_bound, shifts, head_count):
    squashed = jax.nn.sigmoid(pre_act.astype(jnp.float32))
    key_rows = (1.0 - lower_bound)[None, :] * (1.0 - squashed)
    key_rows = key_rows.reshape(key_rows.shape[0], head_count, key_rows.shape[1] // head_count)
    log_decay = jnp.log1p(-key_rows) + shifts[:, :, None]
    return (key_rows, log_decay)

def sweep_blocks(queries, key_rows, values, log_decay, blk_rows):
    token_count, head_count, key_width = queries.shape
    value_width = values.shape[2]
    block_count = token_count // blk_rows
    lower_mask = jnp.tril(jnp.ones((blk_rows, blk_rows), jnp.float32))

    def to_blocks(array):
        return array.reshape(block_count, blk_rows, head_count, array.shape[2])

    def advance(carried, block):
        states, offset = carried
        block_q, block_k, block_v, block_g = block
        running = jnp.cumsum(block_g, axis=0)
        query_grown = block_q * jnp.exp(running)
        key_shrunk = block_k * jnp.exp(-running)
        scores = jnp.einsum('thd,shd->hts', query_grown, key_shrunk, precision=PRECISE) * lower_mask[None]
        result = jnp.einsum('hts,shv->thv', scores, block_v, precision=PRECISE) + jnp.einsum('thd,hdv->thv', query_grown, states, precision=PRECISE)
        block_end = running[-1]
        states = jnp.exp(block_end)[:, :, None] * states + jnp.einsum('shd,shv->hdv', block_k * jnp.exp(block_end[None] - running), block_v, precision=PRECISE)
        return ((states, offset + block_end), (result, offset[None] + running))
    starting = (jnp.zeros((head_count, key_width, value_width), jnp.float32), jnp.zeros((head_count, key_width), jnp.float32))
    blocks_in = (to_blocks(queries), to_blocks(key_rows), to_blocks(values), to_blocks(log_decay))
    (states, totals), (results, cumulative) = lax.scan(advance, starting, blocks_in)
    return (results.reshape(token_count, head_count, value_width), cumulative.reshape(token_count, head_count, key_width), totals, states)

def slot_positions(route_rows, expert_count, capacity):
    flattened = route_rows.reshape(-1)
    onehot = (flattened[:, None] == jnp.arange(expert_count, dtype=jnp.int32)[None, :]).astype(jnp.int32)
    before = jnp.cumsum(onehot, axis=0) - onehot
    slot_rank = lax.optimization_barrier(jnp.sum(before * onehot, axis=1))
    return (flattened * capacity + slot_rank).reshape(route_rows.shape).astype(jnp.int32)

def reference(mix_tokens, mix_gain, w_query, w_forget_fwd, w_forget_bwd, w_value, decay_floor, decay_shift, head_gain, w_out, moe_tokens, moe_gain, routes, route_logits, w_expert_gate, w_expert_up, w_expert_down):
    normed = rms_rows(mix_tokens, mix_gain).astype(jnp.bfloat16)

    def project(weight):
        return jnp.dot(normed, weight, preferred_element_type=jnp.float32).astype(jnp.bfloat16)
    queries = jax.nn.silu(project(w_query).astype(jnp.float32)).reshape(ROWS, HEADS, DK)
    values = project(w_value).astype(jnp.float32).reshape(ROWS, HEADS, DV)
    keys_fwd, forward_log_decay = decay_terms(project(w_forget_fwd), decay_floor, decay_shift, HEADS)
    keys_bwd, logs_bwd = decay_terms(project(w_forget_bwd), decay_floor, decay_shift, HEADS)
    out_fwd = sweep_blocks(queries, keys_fwd, values, forward_log_decay, 128)[0]
    out_bwd = sweep_blocks(jnp.flip(queries, 0), jnp.flip(keys_bwd, 0), jnp.flip(values, 0), jnp.flip(logs_bwd, 0), 128)[0]
    combined = out_fwd + jnp.flip(out_bwd, 0)
    readout = rms_rows(combined, head_gain).reshape(ROWS, HEADS * DV).astype(jnp.bfloat16)
    mixed_out = jnp.dot(readout, w_out, preferred_element_type=jnp.float32).astype(jnp.bfloat16)
    normed_moe = rms_rows(moe_tokens, moe_gain).astype(jnp.bfloat16)
    blocks = routes.reshape(N_EP, M_EP, TOPK)
    position = jax.vmap(functools.partial(slot_positions, expert_count=EXPERTS, capacity=CAP))(blocks)
    local_rows = jnp.arange(TOPK * M_EP, dtype=jnp.int32) // TOPK

    def slot_table(block_pos, source):
        filled = jnp.full((EXPERTS * CAP,), MROWS, jnp.int32)
        return filled.at[block_pos.reshape(-1)].set(source * M_EP + local_rows)
    tables = jax.vmap(slot_table)(position, jnp.arange(N_EP, dtype=jnp.int32))
    by_expert = tables.reshape(N_EP, EXPERTS, CAP).transpose(1, 0, 2).reshape(EXPERTS, N_EP * CAP)
    padded = jnp.concatenate([normed_moe, jnp.zeros((1, D), jnp.bfloat16)], axis=0)
    group_cols = FF // N_TP

    def expert_rows(expert_args):
        rows_index, gate_weight, up_weight, down_weight = expert_args
        row_data = padded[rows_index]
        gate_acts = jnp.dot(row_data, gate_weight, preferred_element_type=jnp.float32)
        up_acts = jnp.dot(row_data, up_weight, preferred_element_type=jnp.float32)
        hidden = (jax.nn.silu(gate_acts) * up_acts).astype(jnp.bfloat16)
        summed = jnp.zeros((row_data.shape[0], D), jnp.float32)
        for step_index in range(N_TP):
            partial_value = jnp.dot(hidden[:, step_index * group_cols:(step_index + 1) * group_cols], down_weight[step_index * group_cols:(step_index + 1) * group_cols], preferred_element_type=jnp.float32).astype(jnp.bfloat16)
            summed = summed + lax.optimization_barrier(partial_value).astype(jnp.float32)
        return summed.astype(jnp.bfloat16)
    results = lax.map(expert_rows, (by_expert, w_expert_gate, w_expert_up, w_expert_down))
    slot_of = position - blocks * CAP
    sources = jnp.arange(N_EP, dtype=jnp.int32)[:, None, None]
    flat_index = ((blocks * N_EP + sources) * CAP + slot_of).reshape(MROWS, TOPK)
    picked = results.reshape(EXPERTS * N_EP * CAP, D)[flat_index].astype(jnp.float32)
    weights = jax.nn.sigmoid(route_logits - jnp.flip(route_logits, 1))
    moe_out = lax.optimization_barrier(jnp.sum(picked * weights[:, :, None], axis=1)).astype(jnp.bfloat16)
    return (mixed_out, moe_out)
```

```python
import functools

import jax
import jax.numpy as jnp
from jax import lax
from jax.experimental import pallas as pl
from jax.experimental.pallas import tpu as pltpu
from jax.sharding import Mesh
from jax.sharding import PartitionSpec as P

EP = ("ep_0", "ep_1")
EP_TP = ("ep_0", "ep_1", "tp")
EPSILON = 1e-06
F32, BF16 = jnp.float32, jnp.bfloat16
VMEM = pl.BlockSpec(memory_space=pltpu.VMEM)
ANY = pl.BlockSpec(memory_space=pl.ANY)
MESH = pl.DeviceIdType.MESH
BLK = 128
VMEM_MAX = 60 * 1024 * 1024


def dot(a, b):
    return jnp.dot(a, b, preferred_element_type=F32)


def dot_last(a, b):
    return lax.dot_general(a, b, (((1,), (1,)), ((), ())), preferred_element_type=F32)


def dot_first(a, b):
    return lax.dot_general(a, b, (((0,), (0,)), ((), ())), preferred_element_type=F32)


def slot_rows(routes_ref, experts, capacity):
    rows = routes_ref.shape[1]
    first, second = routes_ref[0:1, :], routes_ref[1:2, :]
    names = lax.broadcasted_iota(jnp.int32, (experts, rows), 0)
    is_first = (names == first).astype(F32)
    is_second = (names == second).astype(F32)
    earlier = lax.broadcasted_iota(jnp.int32, (rows, rows), 0) < lax.broadcasted_iota(
        jnp.int32, (rows, rows), 1
    )
    before = dot((is_first + is_second).astype(BF16), earlier.astype(F32).astype(BF16))
    base = names.astype(F32) * float(capacity) + before
    return (
        jnp.sum(is_first * base, axis=0, keepdims=True),
        jnp.sum(is_second * base, axis=0, keepdims=True),
    )


def dispatch_kernel(experts, capacity, x_ref, gain_ref, routes_ref, out_ref, own_ref):
    rows, width = x_ref.shape
    cols = out_ref.shape[1]
    mine = pl.ds(pl.multiple_of(lax.axis_index("tp") * cols, cols), cols)
    gain = gain_ref[:, mine]
    step = 32

    def norm(i, carry):
        at = pl.ds(pl.multiple_of(i * step, step), step)
        x = x_ref[at, :].astype(F32)
        factor = lax.rsqrt(jnp.sum(x * x, axis=-1, keepdims=True) * (1.0 / width) + EPSILON)
        own_ref[at, :] = (x_ref[at, mine].astype(F32) * factor * gain).astype(BF16)
        return carry

    lax.fori_loop(0, rows // step, norm, 0)
    pos_a, pos_b = slot_rows(routes_ref, experts, capacity)
    total = experts * capacity
    chunk = total // 4
    own = own_ref[...]
    for c in range(4):
        slots = (lax.broadcasted_iota(jnp.int32, (chunk, rows), 0) + c * chunk).astype(F32)
        pick = ((slots == pos_a) | (slots == pos_b)).astype(F32).astype(BF16)
        out_ref[c * chunk : (c + 1) * chunk, :] = dot(pick, own).astype(BF16)


def combine_kernel(experts, capacity, back_ref, routes_ref, logits_ref, out_ref):
    rows = routes_ref.shape[1]
    total = experts * capacity
    cols = out_ref.shape[1]
    pos_a, pos_b = slot_rows(routes_ref, experts, capacity)
    la, lb = logits_ref[0:1, :], logits_ref[1:2, :]
    wa, wb = jax.nn.sigmoid(la - lb), jax.nn.sigmoid(lb - la)
    back = back_ref[...]
    for r in range(rows // BLK):
        at = slice(r * BLK, (r + 1) * BLK)

        def column(row):
            return jnp.broadcast_to(row[:, at], (BLK, BLK)).T

        result = None
        for pos, weight in ((pos_a, wa), (pos_b, wb)):
            place = column(pos)
            lanes = lax.broadcasted_iota(jnp.int32, (BLK, BLK), 1)
            picks = [
                (place == (lanes + c * BLK).astype(F32)).astype(F32).astype(BF16)
                for c in range(total // BLK)
            ]
            got = dot(jnp.concatenate(picks, axis=1), back)
            scale = column(weight)
            term = got * jnp.concatenate([scale] * (cols // BLK), axis=1)
            result = term if result is None else result + term
        out_ref[at, :] = result.astype(BF16)


def mixer_kernel(
    x_ref,
    gain_ref,
    wq_ref,
    wf_ref,
    wb_ref,
    wv_ref,
    floor_ref,
    shift_ref,
    out_ref,
    grown_ref,
    s_ref,
    t_ref,
    n_ref,
    q_ref,
    v_ref,
    kf_ref,
    gf_ref,
    kb_ref,
    gb_ref,
    st_ref,
    off_ref,
):
    tile, width = x_ref.shape
    step_id = pl.program_id(0)
    span = 32

    def norm(i, carry):
        at = pl.ds(pl.multiple_of(i * span, span), span)
        x = x_ref[at, :].astype(F32)
        factor = lax.rsqrt(jnp.sum(x * x, axis=-1, keepdims=True) * (1.0 / width) + EPSILON)
        n_ref[at, :] = (x * factor * gain_ref[...]).astype(BF16)
        return carry

    lax.fori_loop(0, tile // span, norm, 0)
    n = n_ref[...]

    def project(w_ref):
        return dot(n, w_ref[...]).astype(BF16).astype(F32)

    at = pl.ds(pl.multiple_of(step_id * tile, tile), tile)
    u = project(wq_ref)
    q_ref[at, :] = u / (1.0 + jnp.exp(-u))
    v_ref[at, :] = project(wv_ref).astype(BF16)
    shift = []
    for j in range(tile // BLK):
        where_at = pl.ds(pl.multiple_of(step_id * tile + j * BLK, BLK), BLK)
        shift.append(
            jnp.concatenate(
                [
                    jnp.broadcast_to(shift_ref[h : h + 1, where_at], (BLK, BLK)).T
                    for h in range(2)
                ],
                axis=1,
            )
        )
    shift = jnp.concatenate(shift, axis=0)
    room = 1.0 - floor_ref[...]
    for w_ref, k_ref, g_ref in ((wf_ref, kf_ref, gf_ref), (wb_ref, kb_ref, gb_ref)):
        key = room * (1.0 - jax.nn.sigmoid(project(w_ref)))
        k_ref[at, :] = key
        g_ref[at, :] = jnp.log1p(-key) + shift

    @pl.when(step_id == pl.num_programs(0) - 1)
    def _():
        blocks = q_ref.shape[0] // BLK
        row = lax.broadcasted_iota(jnp.int32, (BLK, BLK), 0)
        col = lax.broadcasted_iota(jnp.int32, (BLK, BLK), 1)
        st_ref[...] = jnp.zeros_like(st_ref)
        off_ref[...] = jnp.zeros_like(off_ref)
        out_ref[...] = jnp.zeros_like(out_ref)

        def sweep(direction, block, k_ref, g_ref):
            rows = pl.ds(pl.multiple_of(block * BLK, BLK), BLK)
            keep = (col <= row) if direction == 0 else (col >= row)
            tri = keep.astype(F32).astype(BF16)
            g = g_ref[rows, :]
            hi = g.astype(BF16)
            lo = (g - hi.astype(F32)).astype(BF16)
            run = dot(tri, hi) + dot(tri, lo)
            end = run[BLK - 1 : BLK, :] if direction == 0 else run[0:1, :]
            mid = 0.5 * end
            half = jnp.exp(mid)
            qg = q_ref[rows, :] * jnp.exp(run - mid)
            ks = k_ref[rows, :] * jnp.exp(mid - run)
            qfull = qg * half
            kfull = (ks * half).astype(BF16)
            offset = off_ref[direction : direction + 1, :]
            grown_ref[rows, direction * 256 : direction * 256 + 256] = (
                qfull * jnp.exp(offset)
            ).astype(BF16)
            qg, ks, qfull = qg.astype(BF16), ks.astype(BF16), qfull.astype(BF16)
            decay = jnp.exp(end)
            parts = []
            for h in range(2):
                lanes = slice(h * 128, h * 128 + 128)
                v = v_ref[rows, lanes]
                state = st_ref[direction * 2 + h]
                scores = jnp.where(keep, dot_last(qg[:, lanes], ks[:, lanes]), 0.0).astype(BF16)
                parts.append(dot(scores, v) + dot_last(qfull[:, lanes], state.astype(BF16)))
                st_ref[direction * 2 + h] = state * decay[:, lanes] + dot_first(v, kfull[:, lanes])
            out_ref[rows, :] += jnp.concatenate(parts, axis=1)
            off_ref[direction : direction + 1, :] = offset + end

        def both(i, carry):
            sweep(0, i, kf_ref, gf_ref)
            sweep(1, blocks - 1 - i, kb_ref, gb_ref)
            return carry

        lax.fori_loop(0, blocks, both, 0)
        s_ref[...] = st_ref[...].astype(BF16)
        t_ref[...] = jnp.concatenate(
            [off_ref[0:1, 0:128], off_ref[0:1, 128:256], off_ref[1:2, 0:128], off_ref[1:2, 128:256]]
            + [jnp.zeros((4, 128), F32)],
            axis=0,
        )


def finish_kernel(
    s_ref,
    t_ref,
    local_ref,
    grown_ref,
    hgain_ref,
    w_hbm,
    out_ref,
    s1,
    t1,
    s2,
    t2,
    sr,
    tr,
    inc_ref,
    ro_ref,
    rin_ref,
    w_ref,
    send_a,
    recv_a,
    send_b,
    recv_b,
    send_r,
    recv_r,
    w_sem,
):
    z, x, t = lax.axis_index("ep_0"), lax.axis_index("ep_1"), lax.axis_index("tp")
    tp = rin_ref.shape[1] // 256
    w_copy = pltpu.make_async_copy(w_hbm, w_ref, w_sem)
    w_copy.start()
    barrier = pltpu.get_barrier_semaphore()
    for d in range(1, 4):
        pl.semaphore_signal(barrier, inc=1, device_id={"ep_1": lax.rem(x + d, 4)}, device_id_type=MESH)
        pl.semaphore_signal(barrier, inc=1, device_id={"ep_0": lax.rem(z + d, 4)}, device_id_type=MESH)
    for d in range(1, tp):
        pl.semaphore_signal(barrier, inc=1, device_id={"tp": lax.rem(t + d, tp)}, device_id_type=MESH)
    pl.semaphore_wait(barrier, 6 + tp - 1)

    def exchange(axis, me, s_src, t_src, s_dst, t_dst, send, recv):
        copies = []
        for d in range(1, 4):
            for n, (src, dst) in enumerate(((s_src, s_dst), (t_src, t_dst))):
                copies.append(
                    pltpu.make_async_remote_copy(
                        src_ref=src,
                        dst_ref=dst.at[d - 1],
                        send_sem=send.at[2 * d - 2 + n],
                        recv_sem=recv.at[2 * d - 2 + n],
                        device_id={axis: lax.rem(me + d, 4)},
                        device_id_type=MESH,
                    )
                )
        for c in copies:
            c.start()
        for c in copies:
            c.wait_recv()
        return copies

    def state_of(ref, n):
        return ref[n].astype(F32)

    def chain(total, log, use, s, g):
        gate = jnp.where(use, 1.0, 0.0)
        return total + gate * jnp.exp(log) * s, log + gate * g

    def walk(n, me, s_buf, t_buf, behind):
        acc, log = jnp.zeros((128, 128), F32), jnp.zeros((1, 128), F32)
        for d in (1, 2, 3) if behind else (3, 2, 1):
            use = (me >= d) if behind else (me < d)
            acc, log = chain(acc, log, use, s_buf[d - 1, n].astype(F32), t_buf[d - 1, n : n + 1, :])
        return acc, log

    first = exchange("ep_1", x, s_ref, t_ref, s1, t1, send_a, recv_a)
    near = []
    totals = []
    for n in range(4):
        forward = n < 2
        near.append(walk(n, x, s1, t1, forward))
        acc, log = jnp.zeros((128, 128), F32), jnp.zeros((1, 128), F32)
        order = (1, 2, 3) if forward else (3, 2, 1)
        for d in order:
            use = (x < d) if forward else (x >= d)
            acc, log = chain(acc, log, use, s1[d - 1, n].astype(F32), t1[d - 1, n : n + 1, :])
        acc, log = chain(acc, log, True, s_ref[n].astype(F32), t_ref[n : n + 1, :])
        for d in order:
            use = (x >= d) if forward else (x < d)
            acc, log = chain(acc, log, use, s1[d - 1, n].astype(F32), t1[d - 1, n : n + 1, :])
        sr[n] = acc.astype(BF16)
        totals.append(log)
    tr[...] = jnp.concatenate(totals + [jnp.zeros((4, 128), F32)], axis=0)
    second = exchange("ep_0", z, sr, tr, s2, t2, send_b, recv_b)
    for n in range(4):
        far, _ = walk(n, z, s2, t2, n < 2)
        acc, log = near[n]
        inc_ref[n] = (acc + jnp.exp(log) * far).astype(BF16)

    sends = []
    for d in list(range(1, tp)) + [0]:
        peer = lax.rem(t + d, tp)
        rows = pl.ds(pl.multiple_of(peer * 128, 128), 128)
        for h in range(2):
            lanes = slice(h * 128, h * 128 + 128)
            o = (
                local_ref[rows, lanes]
                + dot_last(grown_ref[rows, h * 128 : h * 128 + 128], inc_ref[h])
                + dot_last(grown_ref[rows, 256 + h * 128 : 384 + h * 128], inc_ref[2 + h])
            )
            factor = lax.rsqrt(jnp.mean(o * o, axis=-1, keepdims=True) + EPSILON)
            ro_ref[rows, lanes] = (o * factor * hgain_ref[...]).astype(BF16)
        if d:
            copy = pltpu.make_async_remote_copy(
                src_ref=ro_ref.at[rows, :],
                dst_ref=rin_ref.at[:, pl.ds(pl.multiple_of(t * 256, 256), 256)],
                send_sem=send_r.at[d - 1],
                recv_sem=recv_r.at[d - 1],
                device_id={"tp": peer},
                device_id_type=MESH,
            )
            copy.start()
            sends.append(copy)
    own = pl.ds(pl.multiple_of(t * 128, 128), 128)
    rin_ref[:, pl.ds(pl.multiple_of(t * 256, 256), 256)] = ro_ref[own, :]
    for c in sends:
        c.wait_recv()
    w_copy.wait()
    for n in range(w_ref.shape[1] // 256):
        cols = slice(n * 256, n * 256 + 256)
        out_ref[:, cols] = dot(rin_ref[...], w_ref[:, cols]).astype(BF16)
    for c in first + second + sends:
        c.wait_send()


def params(**more):
    return pltpu.CompilerParams(vmem_limit_bytes=VMEM_MAX, **more)


def body(
    mix_tokens,
    mix_gain,
    w_query,
    w_forget_fwd,
    w_forget_bwd,
    w_value,
    decay_floor,
    decay_shift,
    head_gain,
    w_out,
    moe_tokens,
    moe_gain,
    routes,
    route_logits,
    w_expert_gate,
    w_expert_up,
    w_expert_down,
):
    tp_size = lax.axis_size("tp")
    ep_size = lax.axis_size(EP)
    seg_rows, width = mix_tokens.shape
    token_rows = moe_tokens.shape[0]
    capacity = 3 * token_rows // ep_size
    part_cols = width // tp_size
    slots = ep_size * capacity
    routes_t, logits_t = routes.T, route_logits.T

    outgoing = pl.pallas_call(
        functools.partial(dispatch_kernel, ep_size, capacity),
        out_shape=jax.ShapeDtypeStruct((slots, part_cols), BF16),
        in_specs=[VMEM] * 3,
        out_specs=VMEM,
        scratch_shapes=[pltpu.VMEM((token_rows, part_cols), BF16)],
        compiler_params=params(),
        name="dispatch",
    )(moe_tokens, moe_gain.reshape(1, -1), routes_t)
    arrived = lax.all_to_all(
        outgoing.reshape(ep_size, capacity, part_cols), EP, split_axis=0, concat_axis=0, tiled=True
    )
    pieces = lax.all_gather(arrived, "tp", axis=2, tiled=True)

    tile = 256
    fixed = lambda i: (0, 0)
    local, grown, states, totals = pl.pallas_call(
        mixer_kernel,
        grid=(seg_rows // tile,),
        out_shape=(
            jax.ShapeDtypeStruct((seg_rows, 256), F32),
            jax.ShapeDtypeStruct((seg_rows, 512), BF16),
            jax.ShapeDtypeStruct((4, 128, 128), BF16),
            jax.ShapeDtypeStruct((8, 128), F32),
        ),
        in_specs=[
            pl.BlockSpec((tile, width), lambda i: (i, 0)),
            pl.BlockSpec((1, width), fixed),
            pl.BlockSpec((width, 256), fixed),
            pl.BlockSpec((width, 256), fixed),
            pl.BlockSpec((width, 256), fixed),
            pl.BlockSpec((width, 256), fixed),
            pl.BlockSpec((1, 256), fixed),
            pl.BlockSpec((2, seg_rows), fixed),
        ],
        out_specs=(
            pl.BlockSpec((seg_rows, 256), fixed),
            pl.BlockSpec((seg_rows, 512), fixed),
            pl.BlockSpec((4, 128, 128), lambda i: (0, 0, 0)),
            pl.BlockSpec((8, 128), fixed),
        ),
        scratch_shapes=[
            pltpu.VMEM((tile, width), BF16),
            pltpu.VMEM((seg_rows, 256), F32),
            pltpu.VMEM((seg_rows, 256), BF16),
            pltpu.VMEM((seg_rows, 256), F32),
            pltpu.VMEM((seg_rows, 256), F32),
            pltpu.VMEM((seg_rows, 256), F32),
            pltpu.VMEM((seg_rows, 256), F32),
            pltpu.VMEM((4, 128, 128), F32),
            pltpu.VMEM((8, 256), F32),
        ],
        compiler_params=params(dimension_semantics=("arbitrary",)),
        cost_estimate=pl.CostEstimate(flops=12 * 10**9, bytes_accessed=12 * 2**20, transcendentals=0),
        name="mixer",
    )(
        mix_tokens,
        mix_gain.reshape(1, -1),
        w_query,
        w_forget_fwd,
        w_forget_bwd,
        w_value,
        decay_floor.reshape(1, -1),
        decay_shift.T,
    )
    mixed_out = pl.pallas_call(
        finish_kernel,
        out_shape=jax.ShapeDtypeStruct((seg_rows // tp_size, width), BF16),
        in_specs=[VMEM, VMEM, VMEM, VMEM, VMEM, ANY],
        out_specs=VMEM,
        scratch_shapes=[
            pltpu.VMEM((3, 4, 128, 128), BF16),
            pltpu.VMEM((3, 8, 128), F32),
            pltpu.VMEM((3, 4, 128, 128), BF16),
            pltpu.VMEM((3, 8, 128), F32),
            pltpu.VMEM((4, 128, 128), BF16),
            pltpu.VMEM((8, 128), F32),
            pltpu.VMEM((4, 128, 128), BF16),
            pltpu.VMEM((seg_rows, 256), BF16),
            pltpu.VMEM((seg_rows // tp_size, width), BF16),
            pltpu.VMEM(w_out.shape, BF16),
            pltpu.SemaphoreType.DMA((6,)),
            pltpu.SemaphoreType.DMA((6,)),
            pltpu.SemaphoreType.DMA((6,)),
            pltpu.SemaphoreType.DMA((6,)),
            pltpu.SemaphoreType.DMA((tp_size - 1,)),
            pltpu.SemaphoreType.DMA((tp_size - 1,)),
            pltpu.SemaphoreType.DMA,
        ],
        compiler_params=params(collective_id=1, has_side_effects=True),
        cost_estimate=pl.CostEstimate(flops=12 * 10**9, bytes_accessed=12 * 2**20, transcendentals=0),
        name="finish",
    )(states, totals, local, grown, head_gain.reshape(1, -1), w_out)

    flattened = pieces.reshape(-1, width)
    gate_acts = dot(flattened, w_expert_gate[0])
    up_acts = dot(flattened, w_expert_up[0])
    hidden = (jax.nn.silu(gate_acts) * up_acts).astype(BF16)
    partial_value = dot(hidden, w_expert_down[0])
    summed = lax.psum_scatter(partial_value.astype(BF16), "tp", scatter_dimension=1, tiled=True)
    returned = lax.all_to_all(
        summed.reshape(ep_size, capacity, part_cols), EP, split_axis=0, concat_axis=0, tiled=True
    )
    moe_out = pl.pallas_call(
        functools.partial(combine_kernel, ep_size, capacity),
        out_shape=jax.ShapeDtypeStruct((token_rows, part_cols), BF16),
        in_specs=[VMEM] * 3,
        out_specs=VMEM,
        compiler_params=params(),
        name="combine",
    )(returned.reshape(slots, part_cols), routes_t, logits_t)
    return (mixed_out, moe_out)


def solution(mesh):
    finer = Mesh(mesh.devices.reshape(4, 4, mesh.shape["tp"]), ("ep_0", "ep_1", "tp"))
    return jax.shard_map(
        body,
        mesh=finer,
        in_specs=(
            P(EP, None),
            P(),
            P(None, "tp"),
            P(None, "tp"),
            P(None, "tp"),
            P(None, "tp"),
            P("tp"),
            P(EP, "tp"),
            P(),
            P(),
            P(EP, None),
            P(),
            P(EP, None),
            P(EP, None),
            P(EP, None, "tp"),
            P(EP, None, "tp"),
            P(EP, "tp", None),
        ),
        out_specs=(P(EP_TP, None), P(EP, "tp")),
        check_vma=False,
    )
```
